256 devices in a mesh: ep: 64 (over z, y, core), tp: 4 (over x).
Axes of the slice: x: 4, y: 4, z: 8, core: 2. Of those that a mesh axis runs over, the one named last changes fastest.
Arguments:
- mix_tokens: bfloat16 [65536, 2048], P(('ep', 'tp')), may hold values from -6 to 6
- mix_gain: bfloat16 [2048], replicated, may hold values from 0.099609375 to 1.8984375
- w_branch: bfloat16 [2048, 2048], P(None, 'tp'), may hold values from -0.125 to 0.125
- w_gate_branch: bfloat16 [2048, 2048], P(None, 'tp'), may hold values from -0.125 to 0.125
- conv_taps: bfloat16 [4, 2048], P(None, 'tp'), may hold values from -3 to 3
- recur_gate_w: bfloat16 [32, 64, 64], P('tp'), may hold values from -0.75 to 0.75
- inject_gate_w: bfloat16 [32, 64, 64], P('tp'), may hold values from -0.75 to 0.75
- decay_logit: float32 [2048], P('tp')
- decay_kick: float32 [65536, 32], P('ep', 'tp'), may hold values from -0.7 to 0
- w_mix_out: bfloat16 [2048, 2048], P('tp'), may hold values from -0.125 to 0.125
- moe_tokens: bfloat16 [32768, 2048], P(('ep', 'tp')), may hold values from -6 to 6
- moe_gain: bfloat16 [2048], replicated, may hold values from 0.099609375 to 1.8984375
- expert_ids: int32 [32768, 2], P(('ep', 'tp')), may hold values from 0 to 63, all different within a row; in each aligned block of 128 rows (0 to 127, 128 to 255, ...) at most 8 rows name the same one
- route_weight: float32 [32768, 2], P(('ep', 'tp')), may hold values from 0.1 to 1
- expert_gate_w: bfloat16 [64, 2048, 1024], P('ep', None, 'tp'), may hold values from -0.125 to 0.125
- expert_up_w: bfloat16 [64, 2048, 1024], P('ep', None, 'tp'), may hold values from -0.125 to 0.125
- expert_down_w: bfloat16 [64, 1024, 2048], P('ep', 'tp'), may hold values from -0.1875 to 0.1875
Outputs:
- mixer_out: bfloat16 [65536, 2048], P(('ep', 'tp'))
- expert_out: bfloat16 [32768, 2048], P(('ep', 'tp'))
The draws below stay inside these ranges and needn't reach their ends.
Inputs may be any that keep to these rules, and one draw needn't show every extreme that they name: `expert_ids`: each row names 2 different experts. In each aligned block of 128 rows (the rows of one device) no expert is named more than 8 times, a bound that some block reaches.
All inputs are finite; a program needn't handle non-finite values.
Results may differ from the reference program's by a relative error of at most 0.015.
Values may be sent and summed in bfloat16 or wider, within the bound.
A program may use at most 128 MiB of HBM per device.

```python
import math
import jax
import jax.numpy as jnp
import numpy as np
from jax import lax

D = 2048
RECURRENT_HEADS = 32
HEAD_DIM = 64
B_WIDTH = 2048
CONV = 4
FF = 1024
TOP_K = 2
MIX_DEV = 256
MOE_DEV = 128
MIXER_TOKENS = 65536
MOE_TOKENS = 32768
EXPERTS = 64
CAP = 8
N_TP = 4


def draw_decay_logit(key, part):
    fast_key, rate_key = jax.random.split(jax.random.fold_in(key, 11))
    share = 0.5
    fast_mask = jax.random.uniform(fast_key, (B_WIDTH,), jnp.float32) < share
    unit_draw = jax.random.uniform(rate_key, (B_WIDTH,), jnp.float32)
    fast_rate = jnp.exp(jnp.log(1.0 / 400.0) + unit_draw * jnp.log(400.0 / 120.0))
    slow_rate = jnp.exp(jnp.log(0.05) + unit_draw * jnp.log(2.0)) / MIXER_TOKENS
    step_rate = jnp.where(fast_mask, fast_rate, slow_rate)
    return (-jnp.log(jnp.expm1(step_rate))).astype(jnp.float32)


def draw_decay_kick(key, part):
    rate_key, location_random_key, size_random_key = jax.random.split(jax.random.fold_in(key, 23), 3)
    blocks = MIXER_TOKENS // MIX_DEV
    per_block = jnp.exp(jnp.log(0.5) + jnp.log(4.0) * jax.random.uniform(rate_key, (blocks, 1), jnp.float32))
    block_offset = jnp.repeat(-0.5 * per_block / MIXER_TOKENS, MIX_DEV, axis=0) * jnp.ones((1, RECURRENT_HEADS), jnp.float32)
    spike_locations = jax.random.randint(location_random_key, (3, RECURRENT_HEADS), 0, MIXER_TOKENS)
    spike_depth = jnp.log(jax.random.uniform(size_random_key, (3, RECURRENT_HEADS), jnp.float32, 0.55, 0.8))
    token_position = jnp.arange(MIXER_TOKENS, dtype=jnp.int32)[:, None]
    spike_events = jnp.zeros((MIXER_TOKENS, RECURRENT_HEADS), jnp.float32)
    for index_value in range(3):
        spike_events = spike_events + jnp.where(token_position == spike_locations[index_value][None, :], spike_depth[index_value][None, :], 0.0)
    return (block_offset + spike_events).astype(jnp.float32)


def shard_levels(rng, extent, cuts, smallest, largest):
    level, own = 1.0, jax.random.fold_in(rng, 6)
    for position, shards_of in cuts:
        steps = jnp.exp(jax.random.uniform(jax.random.fold_in(own, position), (shards_of,), jnp.float32, smallest / len(cuts), largest / len(cuts)))
        level = level * jnp.repeat(steps, extent[position] // shards_of).reshape([-1 if axis == position else 1 for axis in range(len(extent))])
    return level


def assign_block(own_key, own, number, rows, count, top, limit, slope):
    order = jax.random.permutation(own_key, count)
    crowded, ordinary = load_shares(count, rows * top, limit, slope, True), load_shares(count, rows * top, limit, slope, False)
    places = jnp.arange(count)

    def named(tallies, offset_by):
        used = int((tallies > 0).sum())
        fixed = max(1, used // 4)
        shifted = fixed + (places - fixed + offset_by * (used - fixed)) % max(1, count - fixed)
        return jnp.zeros((count,), jnp.int32).at[order[jnp.where(places < fixed, places, shifted)]].set(jnp.asarray(tallies, jnp.int32))

    tallies = jnp.where(number % 4 == 0, named(crowded, number // 4), named(ordinary, number - number // 4 - 1))
    mixed = jax.random.permutation(jax.random.fold_in(own, 3), count)
    donor, receiver = mixed[0:count // 2 * 2:2], mixed[1:count // 2 * 2:2]
    margin = jnp.minimum(tallies[donor] - 1, limit - tallies[receiver]) // 2
    margin = jnp.where((donor == order[0]) | (receiver == order[0]) | (tallies[receiver] == 0), 0, jnp.maximum(margin, 0))
    shifted = jax.random.randint(jax.random.fold_in(own, 4), (count // 2,), 0, 1 << 20) % (margin + 1)
    tallies = tallies.at[donor].add(-shifted).at[receiver].add(shifted)
    labels = jnp.searchsorted(jnp.cumsum(tallies), jnp.arange(rows * top), side="right").astype(jnp.int32)
    grid = labels.reshape(top, rows).T
    grid = grid[jax.random.permutation(jax.random.fold_in(own, 1), rows)]
    offset_by = jax.random.randint(jax.random.fold_in(own, 2), (rows, 1), 0, top)
    return jnp.take_along_axis(grid, (jnp.arange(top)[None, :] + offset_by) % top, axis=1)


def load_shares(number_of, total, bound, slope, full):
    weights = [(1 << 20) // math.isqrt(rank ** slope) + 1 for rank in range(1, number_of + 1)]
    largest = bound if full else min(bound, max(-(-total // number_of), total * weights[0] // sum(weights)))
    least = 1 if total - largest >= number_of - 1 else 0
    counts, spare = [largest] + [least] * (number_of - 1), total - largest - least * (number_of - 1)
    while spare > 0:
        candidates = [i for i in range(1, number_of) if counts[i] < largest] or [i for i in range(1, number_of) if counts[i] < bound]
        pool, left = sum([weights[i] for i in candidates]), spare
        for i in candidates:
            addition = min(bound - counts[i], max(1, left * weights[i] // pool), spare)
            counts[i] = counts[i] + addition
            spare = spare - addition
    return np.array(counts)


def centred(own_key, extent, width, bound, pieces=(), kind=jnp.bfloat16):
    drawn = jax.random.normal(own_key, extent, jnp.float32) * width
    if len(pieces) > 0:
        drawn = shard_levels(own_key, extent, pieces, -0.22, 0.18) * drawn
    return jnp.clip(drawn, min=-bound, max=bound).astype(kind)


def setup_inputs(seed: int = 0) -> dict:
    streams_of = jax.random.split(jax.random.key(seed), 18)
    mix_tokens = centred(streams_of[0], (MIXER_TOKENS, D), 1.0, 6.0, ((0, 256),))
    mix_gain = jnp.clip(1.0 + 0.18 * jax.random.normal(streams_of[1], (D,), jnp.float32), 0.099609375, 1.8984375).astype(jnp.bfloat16)
    w_branch = centred(streams_of[2], (D, B_WIDTH), D ** -0.5, 0.125, ((1, 4),))
    w_gate_branch = centred(streams_of[3], (D, B_WIDTH), D ** -0.5, 0.125, ((1, 4),))
    conv_taps = centred(streams_of[4], (CONV, B_WIDTH), CONV ** -0.5, 3.0, ((1, 4),))
    recur_gate_w = centred(streams_of[5], (RECURRENT_HEADS, HEAD_DIM, HEAD_DIM), HEAD_DIM ** -0.5, 0.75, ((0, 4),))
    inject_gate_w = centred(streams_of[6], (RECURRENT_HEADS, HEAD_DIM, HEAD_DIM), HEAD_DIM ** -0.5, 0.75, ((0, 4),))
    decay_logit = draw_decay_logit(jax.random.fold_in(streams_of[17], 71), 0)
    decay_kick = draw_decay_kick(jax.random.fold_in(streams_of[17], 71), 0)
    w_mix_out = centred(streams_of[9], (B_WIDTH, D), B_WIDTH ** -0.5, 0.125, ((0, 4),))
    moe_tokens = centred(streams_of[10], (MOE_TOKENS, D), 1.0, 6.0, ((0, 256),))
    moe_gain = jnp.clip(1.0 + 0.18 * jax.random.normal(streams_of[11], (D,), jnp.float32), 0.099609375, 1.8984375).astype(jnp.bfloat16)
    expert_ids_keys = jax.random.split(jax.random.fold_in(streams_of[12], 1), MOE_TOKENS // MOE_DEV)
    expert_ids_turns = jax.random.permutation(jax.random.fold_in(streams_of[12], 3), MOE_TOKENS // MOE_DEV)
    expert_ids = jax.vmap(lambda own, number: assign_block(jax.random.fold_in(streams_of[12], 2), own, number, MOE_DEV, EXPERTS, TOP_K, CAP, 1))(expert_ids_keys, expert_ids_turns).reshape((MOE_TOKENS, TOP_K))
    route_weight = jnp.clip(jnp.exp(math.log(1.0) - 2.3025851 * jax.random.uniform(streams_of[13], (MOE_TOKENS, TOP_K), jnp.float32) ** shard_levels(streams_of[13], (MOE_TOKENS, TOP_K), ((0, 256),), -0.2, 0.2)), 0.1, 1.0)
    expert_gate_w = centred(streams_of[14], (EXPERTS, D, FF), D ** -0.5, 0.125, ((0, 64), (2, 4)))
    expert_up_w = centred(streams_of[15], (EXPERTS, D, FF), D ** -0.5, 0.125, ((0, 64), (2, 4)))
    expert_down_w = centred(streams_of[16], (EXPERTS, FF, D), FF ** -0.5, 0.1875, ((0, 64), (1, 4)))
    return dict(mix_tokens=mix_tokens, mix_gain=mix_gain, w_branch=w_branch, w_gate_branch=w_gate_branch, conv_taps=conv_taps, recur_gate_w=recur_gate_w, inject_gate_w=inject_gate_w, decay_logit=decay_logit, decay_kick=decay_kick, w_mix_out=w_mix_out, moe_tokens=moe_tokens, moe_gain=moe_gain, expert_ids=expert_ids, route_weight=route_weight, expert_gate_w=expert_gate_w, expert_up_w=expert_up_w, expert_down_w=expert_down_w)


epsilon = 1e-06
gate_const = 8.0

def norm_rows(values, gain_vec):
    value_f32 = values.astype(jnp.float32)
    inv_scale = lax.rsqrt(lax.optimization_barrier(jnp.mean(value_f32 * value_f32, axis=-1, keepdims=True)) + epsilon)
    return (value_f32 * inv_scale * gain_vec.astype(jnp.float32)).astype(jnp.bfloat16)

def chain_link(earlier, later):
    return (later[0] * earlier[0], later[0] * earlier[1] + later[1])

def reference(mix_tokens, mix_gain, w_branch, w_gate_branch, conv_taps, recur_gate_w, inject_gate_w, decay_logit, decay_kick, w_mix_out, moe_tokens, moe_gain, expert_ids, route_weight, expert_gate_w, expert_up_w, expert_down_w):
    mixer_in = norm_rows(mix_tokens, mix_gain)
    branch_x = jnp.dot(mixer_in, w_branch, preferred_element_type=jnp.float32).astype(jnp.bfloat16)
    branch_gate = jnp.dot(mixer_in, w_gate_branch, preferred_element_type=jnp.float32).astype(jnp.bfloat16)
    branch_f32 = branch_x.astype(jnp.float32)
    tap_values = conv_taps.astype(jnp.float32)
    padded = jnp.pad(branch_f32, ((CONV - 1, 0), (0, 0)))
    conv_out = tap_values[CONV - 1] * branch_f32
    for index_value in range(CONV - 1):
        conv_out = conv_out + tap_values[index_value] * padded[index_value:index_value + MIXER_TOKENS]
    conv_low = lax.optimization_barrier(conv_out.astype(jnp.bfloat16))
    low_heads = conv_low.astype(jnp.float32).reshape(MIXER_TOKENS, RECURRENT_HEADS, HEAD_DIM)
    recur = jax.nn.sigmoid(jnp.einsum('thi,hij->thj', low_heads, recur_gate_w.astype(jnp.float32)).reshape(MIXER_TOKENS, B_WIDTH))
    inject = jax.nn.sigmoid(jnp.einsum('thi,hij->thj', low_heads, inject_gate_w.astype(jnp.float32)).reshape(MIXER_TOKENS, B_WIDTH))
    slowness = jax.nn.softplus(-decay_logit)
    kick_wide = jnp.repeat(decay_kick, HEAD_DIM, axis=1)
    log_decay = -gate_const * recur * slowness[None, :] + kick_wide
    drive = jnp.sqrt(-jnp.expm1(2.0 * log_decay)) * inject * conv_out
    _, state = lax.associative_scan(chain_link, (jnp.exp(log_decay), drive), axis=0)
    mixed = (state * jax.nn.gelu(branch_gate.astype(jnp.float32))).astype(jnp.bfloat16)
    col_count = B_WIDTH // N_TP
    summed = jnp.zeros((MIXER_TOKENS, D), jnp.float32)
    for group in range(N_TP):
        piece = jnp.dot(mixed[:, group * col_count:(group + 1) * col_count], w_mix_out[group * col_count:(group + 1) * col_count], preferred_element_type=jnp.float32)
        summed = summed + lax.optimization_barrier(piece.astype(jnp.bfloat16)).astype(jnp.float32)
    mixer_out = summed.astype(jnp.bfloat16)
    moe_in = norm_rows(moe_tokens, moe_gain)
    blocks = MOE_TOKENS // MOE_DEV
    route_ids = expert_ids.reshape(blocks, MOE_DEV * TOP_K)
    onehot = (route_ids[:, :, None] == jnp.arange(EXPERTS, dtype=jnp.int32)[None, None, :]).astype(jnp.int32)
    earlier_count = jnp.cumsum(onehot, axis=1) - onehot
    slot_index = lax.optimization_barrier(jnp.sum(earlier_count * onehot, axis=2))
    per_expert = blocks * CAP
    slot_target = (route_ids * per_expert + jnp.arange(blocks, dtype=jnp.int32)[:, None] * CAP + slot_index).reshape(-1).astype(jnp.int32)
    source = jnp.repeat(moe_in, TOP_K, axis=0)
    buffer = jnp.zeros((EXPERTS * per_expert, D), jnp.bfloat16).at[slot_target].set(source)
    quarter = FF // N_TP

    def run_expert(operands):
        expert_rows, gate_mat, up_mat, down_mat = operands
        hidden = (jax.nn.silu(jnp.dot(expert_rows, gate_mat, preferred_element_type=jnp.float32)) * jnp.dot(expert_rows, up_mat, preferred_element_type=jnp.float32)).astype(jnp.bfloat16)
        summed_rows = jnp.zeros((expert_rows.shape[0], D), jnp.float32)
        for group in range(N_TP):
            piece = jnp.dot(hidden[:, group * quarter:(group + 1) * quarter], down_mat[group * quarter:(group + 1) * quarter], preferred_element_type=jnp.float32)
            summed_rows = summed_rows + lax.optimization_barrier(piece.astype(jnp.bfloat16)).astype(jnp.float32)
        return summed_rows.astype(jnp.bfloat16)
    results = lax.map(run_expert, (buffer.reshape(EXPERTS, per_expert, D), expert_gate_w, expert_up_w, expert_down_w))
    results = results.reshape(EXPERTS * per_expert, D)
    picked = results[slot_target].astype(jnp.float32).reshape(MOE_TOKENS, TOP_K, D)
    expert_out = lax.optimization_barrier(jnp.sum(picked * route_weight[:, :, None], axis=1)).astype(jnp.bfloat16)
    return (mixer_out, expert_out)
```

```python
import functools

import jax
import jax.numpy as jnp
from jax import lax
from jax.experimental import pallas as pl
from jax.experimental.pallas import tpu as pltpu
from jax.sharding import Mesh
from jax.sharding import PartitionSpec as P

EP = ("ep_0", "ep_1", "ep_2")
EP_TP = ("ep_0", "ep_1", "ep_2", "tp")
MESH = pl.DeviceIdType.MESH
F32 = jnp.float32
BF16 = jnp.bfloat16

epsilon = 1e-06
gate_const = 8.0
VMEM = pl.BlockSpec(memory_space=pltpu.VMEM)
ANY = pl.BlockSpec(memory_space=pl.ANY)


def dot(a, b):
    return jnp.dot(a, b, preferred_element_type=F32)


def place():
    return tuple(lax.axis_index(name) for name in EP_TP)


def ep_coords(e):
    return (e // 8, (e // 2) % 4, e % 2)


def normed(values, gain_row):
    value = values.astype(F32)
    inv = lax.rsqrt(jnp.mean(value * value, axis=-1, keepdims=True) + epsilon)
    return (value * inv * gain_row.astype(F32)).astype(BF16)


def pre_kernel(mix, mix_gain, moe, moe_gain, ids, weight, rows, outgoing, table):
    step = 64

    def norm_step(i, carry):
        at = pl.ds(pl.multiple_of(i * step, step), step)
        rows[at, :] = normed(mix[at, :], mix_gain[...])
        return carry

    lax.fori_loop(0, mix.shape[0] // step, norm_step, 0)
    count = moe.shape[0]
    slots = outgoing.shape[0]
    experts = 64
    room = slots // experts
    moe_in = normed(moe[...], moe_gain[...])
    named = lax.broadcasted_iota(jnp.int32, (count, experts), 1)
    picks = [ids[:, k : k + 1] for k in range(2)]
    hot = [(named == p).astype(F32) for p in picks]
    below = lax.broadcasted_iota(jnp.int32, (count, count), 1) < lax.broadcasted_iota(
        jnp.int32, (count, count), 0
    )
    earlier = dot(below.astype(F32).astype(BF16), (hot[0] + hot[1]).astype(BF16))
    slot = [
        picks[k] * room + jnp.sum(earlier * hot[k], axis=1, keepdims=True).astype(jnp.int32)
        for k in range(2)
    ]
    lanes = lax.broadcasted_iota(jnp.int32, (count, slots), 1)
    here = [(lanes == s).astype(F32) for s in slot]
    spread = (here[0] + here[1]).astype(BF16)
    outgoing[...] = lax.dot_general(
        spread, moe_in, (((0,), (0,)), ((), ())), preferred_element_type=F32
    ).astype(BF16)
    table[...] = (here[0] * weight[:, 0:1] + here[1] * weight[:, 1:2]).astype(BF16)


def pre(mix, mix_gain, moe, moe_gain, ids, weight):
    slots = 8 * 64
    return pl.pallas_call(
        pre_kernel,
        name="pre",
        out_shape=(
            jax.ShapeDtypeStruct(mix.shape, BF16),
            jax.ShapeDtypeStruct((slots, moe.shape[1]), BF16),
            jax.ShapeDtypeStruct((moe.shape[0], slots), BF16),
        ),
        in_specs=[VMEM] * 6,
        out_specs=(VMEM,) * 3,
        cost_estimate=pl.CostEstimate(
            flops=4_000_000_000, bytes_accessed=8_000_000, transcendentals=0
        ),
        compiler_params=pltpu.CompilerParams(vmem_limit_bytes=56 * 2**20),
    )(mix, mix_gain, moe, moe_gain, ids, weight)


def gather_kernel(own, out, rim, send, recv, keep):
    z, y, c, t = place()
    n = 4
    right, left = lax.rem(t + 1, n), lax.rem(t + n - 1, n)
    e = z * 8 + y * 2 + c
    before = ep_coords(lax.rem(e + 63, 64))
    after = ep_coords(lax.rem(e + 1, 64))
    barrier = pltpu.get_barrier_semaphore()
    for who in (right, left):
        pl.semaphore_signal(barrier, inc=1, device_id=(z, y, c, who), device_id_type=MESH)
    pl.semaphore_signal(barrier, inc=1, device_id=(*before, n - 1), device_id_type=MESH)

    @pl.when(t == n - 1)
    def _():
        for k in range(n):
            pl.semaphore_signal(barrier, inc=1, device_id=(*after, k), device_id_type=MESH)
        pl.semaphore_wait(barrier, n + 3)

    @pl.when(t < n - 1)
    def _():
        pl.semaphore_wait(barrier, 3)

    half = own.shape[0] // 2
    parts = (pl.ds(0, half), pl.ds(half, half))
    tail = pl.ds(own.shape[0] - 16, 16)
    mine = pltpu.make_async_copy(own, out.at[t], keep)
    mine.start()

    def piece(k, part, src, block, who):
        return pltpu.make_async_remote_copy(
            src_ref=src,
            dst_ref=out.at[block, part],
            send_sem=send.at[k],
            recv_sem=recv.at[k],
            device_id=(z, y, c, who),
            device_id_type=MESH,
        )

    def rim_copy(k):
        return pltpu.make_async_remote_copy(
            src_ref=own.at[tail],
            dst_ref=rim,
            send_sem=send.at[6 + k],
            recv_sem=recv.at[6],
            device_id=(*after, k),
            device_id_type=MESH,
        )

    r0 = piece(0, parts[0], own.at[parts[0]], t, right)
    l1 = piece(1, parts[1], own.at[parts[1]], t, left)
    r1 = piece(2, parts[1], own.at[parts[1]], t, right)
    l0 = piece(3, parts[0], own.at[parts[0]], t, left)
    for copy in (r0, l1, r1, l0):
        copy.start()

    @pl.when(t == n - 1)
    def _():
        for k in range(n):
            rim_copy(k).start()

    r0.wait_recv()
    fr = piece(4, parts[0], out.at[left, parts[0]], left, right)
    fr.start()
    l1.wait_recv()
    fl = piece(5, parts[1], out.at[right, parts[1]], right, left)
    fl.start()
    r1.wait_recv()
    l0.wait_recv()
    fr.wait_recv()
    fl.wait_recv()
    rim_copy(0).wait_recv()
    for copy in (r0, l1, r1, l0, fr, fl):
        copy.wait_send()

    @pl.when(t == n - 1)
    def _():
        for k in range(n):
            rim_copy(k).wait_send()

    mine.wait()


def gather_rows(rows):
    return pl.pallas_call(
        gather_kernel,
        name="gather_rows",
        out_shape=(
            jax.ShapeDtypeStruct((4, *rows.shape), BF16),
            jax.ShapeDtypeStruct((16, rows.shape[1]), BF16),
        ),
        in_specs=[VMEM],
        out_specs=(ANY, ANY),
        scratch_shapes=[
            pltpu.SemaphoreType.DMA((10,)),
            pltpu.SemaphoreType.DMA((7,)),
            pltpu.SemaphoreType.DMA,
        ],
        cost_estimate=pl.CostEstimate(
            flops=40_000_000_000, bytes_accessed=8_000_000, transcendentals=0
        ),
        compiler_params=pltpu.CompilerParams(
            collective_id=1, has_side_effects=True, vmem_limit_bytes=56 * 2**20
        ),
    )(rows)


def mid_kernel(
    blocks, rim, w_x, w_g, taps, maps, slow, kick, widen, gate, state, decay, last, ext, pre_act
):
    rows, cols = state.shape
    first = lax.axis_index("ep_0") + lax.axis_index("ep_1") + lax.axis_index("ep_2") == 0
    head = dot(rim[...], w_x[...])[8:16].astype(BF16).astype(F32)
    ext[0:8, :] = jnp.where(first, 0.0, head)
    big = 256

    def project(i, carry):
        base = pl.multiple_of(i * big, big)
        x = blocks[i]
        ext[pl.ds(base + 8, big), :] = dot(x, w_x[...]).astype(BF16).astype(F32)
        gate[pl.ds(base, big), :] = dot(x, w_g[...]).astype(BF16)
        return carry

    lax.fori_loop(0, rows // big, project, 0)
    step = 128
    wide = 128
    lane8 = lax.broadcasted_iota(jnp.int32, (step // 8, 8, wide), 1)
    for j in range(cols // wide):
        lanes = slice(j * wide, (j + 1) * wide)

        def convolve(i, carry):
            base = pl.multiple_of(i * big, big)
            window = ext[pl.ds(base, big + 8), lanes]
            total = taps[3:4, lanes] * window[8:]
            for k in range(3):
                total = total + taps[k : k + 1, lanes] * pltpu.roll(window, 3 - k, 0)[8:]
            state[pl.ds(base, big), lanes] = total
            pre_act[pl.ds(base, big), :] = dot(total.astype(BF16), maps[j])
            return carry

        lax.fori_loop(0, rows // big, convolve, 0)

        def gates(i, carry):
            base = pl.multiple_of(i * step, step)
            at = pl.ds(base, step)
            recur = jax.nn.sigmoid(pre_act[at, :wide])
            inject = jax.nn.sigmoid(pre_act[at, wide:])
            k = kick[at, :]
            k_hi = k.astype(BF16)
            k_lo = (k - k_hi.astype(F32)).astype(BF16)
            kicks = dot(k_hi, widen[:, lanes]) + dot(k_lo, widen[:, lanes])
            ld = -gate_const * recur * slow[:, lanes] + kicks
            series = 1.0 + ld * (1.0 / 6.0)
            for q in (5.0, 4.0, 3.0, 2.0):
                series = 1.0 + ld * (1.0 / q) * series
            em = jnp.where(ld > -0.25, ld * series, jnp.exp(ld) - 1.0)
            a = (1.0 + em).reshape(step // 8, 8, wide)
            d = jnp.sqrt(-em * (2.0 + em)) * inject * state[at, lanes]
            d = d.reshape(step // 8, 8, wide)
            for shift in (1, 2, 4):
                inside = lane8 >= shift
                a_before = jnp.where(inside, pltpu.roll(a, shift, 1), 1.0)
                d_before = jnp.where(inside, pltpu.roll(d, shift, 1), 0.0)
                d = a * d_before + d
                a = a * a_before
            state[at, lanes] = d.reshape(step, wide)
            decay[at, lanes] = a.reshape(step, wide)
            return carry

        lax.fori_loop(0, rows // step, gates, 0)

    def chain(g, carry):
        p, h = carry
        at = pl.ds(pl.multiple_of(g * 8, 8), 8)
        a = decay[at, :]
        new_h = state[at, :] + a * h
        new_p = a * p
        state[at, :] = new_h
        decay[at, :] = new_p
        return (
            jnp.broadcast_to(new_p[7:8], (8, cols)),
            jnp.broadcast_to(new_h[7:8], (8, cols)),
        )

    p, h = lax.fori_loop(
        0,
        rows // 8,
        chain,
        (jnp.ones((8, cols), F32), jnp.zeros((8, cols), F32)),
        unroll=4,
    )
    for j in range(cols // wide):
        last[j : j + 1, :] = p[0:1, j * wide : (j + 1) * wide]
        last[4 + j : 5 + j, :] = h[0:1, j * wide : (j + 1) * wide]


def mid(blocks, rim, w_x, w_g, taps, maps, slow, kick, widen):
    rows = blocks.shape[0] * blocks.shape[1]
    cols = w_x.shape[1]
    return pl.pallas_call(
        mid_kernel,
        name="mid",
        out_shape=(
            jax.ShapeDtypeStruct((rows, cols), BF16),
            jax.ShapeDtypeStruct((rows, cols), F32),
            jax.ShapeDtypeStruct((rows, cols), F32),
            jax.ShapeDtypeStruct((8, 128), F32),
        ),
        in_specs=[VMEM] * 9,
        out_specs=(VMEM,) * 4,
        scratch_shapes=[pltpu.VMEM((rows + 8, cols), F32), pltpu.VMEM((rows, 256), F32)],
        cost_estimate=pl.CostEstimate(
            flops=14_000_000_000, bytes_accessed=16_000_000, transcendentals=0
        ),
        compiler_params=pltpu.CompilerParams(vmem_limit_bytes=56 * 2**20),
    )(blocks, rim, w_x, w_g, taps, maps, slow, kick, widen)


def carry_kernel(own, out, along, around, send, recv_z, recv_p):
    z, y, c, t = place()
    plane = y * 2 + c

    def z_peer(d):
        return (lax.rem(z + d, 8), y, c, t)

    def p_peer(d):
        other = lax.rem(plane + d, 8)
        return (z, other // 2, other % 2, t)

    barrier = pltpu.get_barrier_semaphore()
    for d in range(1, 8):
        pl.semaphore_signal(barrier, inc=1, device_id=z_peer(d), device_id_type=MESH)
        pl.semaphore_signal(barrier, inc=1, device_id=p_peer(d), device_id_type=MESH)
    along[z] = own[...]
    pl.semaphore_wait(barrier, 14)

    def z_copy(d):
        return pltpu.make_async_remote_copy(
            src_ref=own,
            dst_ref=along.at[z],
            send_sem=send.at[d - 1],
            recv_sem=recv_z.at[d - 1],
            device_id=z_peer(d),
            device_id_type=MESH,
        )

    def p_copy(d):
        return pltpu.make_async_remote_copy(
            src_ref=along,
            dst_ref=around.at[plane],
            send_sem=send.at[6 + d],
            recv_sem=recv_p.at[d - 1],
            device_id=p_peer(d),
            device_id_type=MESH,
        )

    order = (4, 3, 5, 2, 6, 1, 7)
    for d in order:
        z_copy(d).start()
    for d in range(1, 8):
        z_copy(d).wait_recv()
    for d in order:
        p_copy(d).start()
    around[plane] = along[...]
    for d in range(1, 8):
        p_copy(d).wait_recv()
    me = z * 8 + plane
    h = jnp.zeros((4, 128), F32)
    for zz in range(8):
        for q in range(8):
            passed = zz * 8 + q < me
            h = jnp.where(passed, around[q, zz, 0:4, :] * h + around[q, zz, 4:8, :], h)
    out[...] = h
    for d in range(1, 8):
        z_copy(d).wait_send()
        p_copy(d).wait_send()


def carried_state(last):
    return pl.pallas_call(
        carry_kernel,
        name="carry",
        out_shape=jax.ShapeDtypeStruct((4, 128), F32),
        in_specs=[VMEM],
        out_specs=VMEM,
        scratch_shapes=[
            pltpu.VMEM((8, 8, 128), F32),
            pltpu.VMEM((8, 8, 8, 128), F32),
            pltpu.SemaphoreType.DMA((14,)),
            pltpu.SemaphoreType.DMA((7,)),
            pltpu.SemaphoreType.DMA((7,)),
        ],
        cost_estimate=pl.CostEstimate(
            flops=10_000_000_000, bytes_accessed=1_000_000, transcendentals=0
        ),
        compiler_params=pltpu.CompilerParams(
            collective_id=2, has_side_effects=True, vmem_limit_bytes=56 * 2**20
        ),
    )(last)


def out_kernel(state, decay, gate, carry, w_out, partial):
    big = 256

    def block(i, nothing):
        at = pl.ds(pl.multiple_of(i * big, big), big)
        full = state[at, :] + decay[at, :] * carry[...]
        mixed = (full * jax.nn.gelu(gate[at, :].astype(F32))).astype(BF16)
        partial[i] = dot(mixed, w_out[...]).astype(BF16)
        return nothing

    lax.fori_loop(0, partial.shape[0], block, 0)


def out_partial(state, decay, gate, carry, w_out):
    return pl.pallas_call(
        out_kernel,
        name="out_partial",
        out_shape=jax.ShapeDtypeStruct((4, 256, w_out.shape[1]), BF16),
        in_specs=[VMEM] * 5,
        out_specs=VMEM,
        cost_estimate=pl.CostEstimate(
            flops=4_000_000_000, bytes_accessed=12_000_000, transcendentals=0
        ),
        compiler_params=pltpu.CompilerParams(vmem_limit_bytes=56 * 2**20),
    )(state, decay, gate, carry, w_out)


def sum_kernel(partial, out, far, near, joined, send, recv):
    z, y, c, t = place()
    n = 4
    right, left = lax.rem(t + 1, n), lax.rem(t + n - 1, n)
    across = lax.rem(t + 2, n)
    barrier = pltpu.get_barrier_semaphore()
    for who in (right, left):
        pl.semaphore_signal(barrier, inc=1, device_id=(z, y, c, who), device_id_type=MESH)
    pl.semaphore_wait(barrier, 2)
    half = out.shape[0] // 2
    parts = (pl.ds(0, half), pl.ds(half, half))

    def piece(k, src, dst, who):
        return pltpu.make_async_remote_copy(
            src_ref=src,
            dst_ref=dst,
            send_sem=send.at[k],
            recv_sem=recv.at[k],
            device_id=(z, y, c, who),
            device_id_type=MESH,
        )

    peers = (right, left)
    first = [piece(s, partial.at[across, parts[s]], far.at[s], peers[s]) for s in range(2)]
    plain = [
        piece(2 + s, partial.at[peers[s], parts[1 - s]], near.at[s, parts[1 - s]], peers[s])
        for s in range(2)
    ]
    summed = [piece(4 + s, joined.at[s], near.at[s, parts[s]], peers[s]) for s in range(2)]
    for copy in first + plain:
        copy.start()
    step = 32
    for s in range(2):
        first[s].wait_recv()

        def join(i, nothing, s=s):
            at = pl.ds(pl.multiple_of(i * step, step), step)
            of = pl.ds(pl.multiple_of(s * half + i * step, step), step)
            joined[s, at, :] = (
                far[s, at, :].astype(F32) + partial[peers[s], of, :].astype(F32)
            ).astype(BF16)
            return nothing

        lax.fori_loop(0, half // step, join, 0)
        summed[s].start()
    for s in range(2):
        plain[s].wait_recv()
        summed[s].wait_recv()

    def total(i, nothing):
        at = pl.ds(pl.multiple_of(i * step, step), step)
        out[at, :] = (
            partial[t, at, :].astype(F32)
            + near[0, at, :].astype(F32)
            + near[1, at, :].astype(F32)
        ).astype(BF16)
        return nothing

    lax.fori_loop(0, out.shape[0] // step, total, 0)
    for copy in first + plain + summed:
        copy.wait_send()


def sum_over_tp(partial):
    _, rows, width = partial.shape
    return pl.pallas_call(
        sum_kernel,
        name="sum_over_tp",
        out_shape=jax.ShapeDtypeStruct((rows, width), BF16),
        in_specs=[VMEM],
        out_specs=VMEM,
        scratch_shapes=[
            pltpu.VMEM((2, rows // 2, width), BF16),
            pltpu.VMEM((2, rows, width), BF16),
            pltpu.VMEM((2, rows // 2, width), BF16),
            pltpu.SemaphoreType.DMA((6,)),
            pltpu.SemaphoreType.DMA((6,)),
        ],
        cost_estimate=pl.CostEstimate(
            flops=40_000_000_000, bytes_accessed=8_000_000, transcendentals=0
        ),
        compiler_params=pltpu.CompilerParams(
            collective_id=3, has_side_effects=True, vmem_limit_bytes=56 * 2**20
        ),
    )(partial)


def ffn_kernel(rows, w_gate, w_up, w_down, out, total):
    g = pl.program_id(0)
    big = 256

    def block(i, nothing):
        at = pl.ds(pl.multiple_of(i * big, big), big)
        x = rows[at, :]
        hidden = (jax.nn.silu(dot(x, w_gate[0])) * dot(x, w_up[0])).astype(BF16)
        new = dot(hidden, w_down[0])

        @pl.when(g == 0)
        def _():
            total[at, :] = new

        @pl.when(g > 0)
        def _():
            total[at, :] += new

        @pl.when(g == pl.num_programs(0) - 1)
        def _():
            out[at, :] = total[at, :].astype(BF16)

        return nothing

    lax.fori_loop(0, rows.shape[0] // big, block, 0)


def ffn(rows, w_gate, w_up, w_down):
    groups, width, quarter = w_gate.shape
    return pl.pallas_call(
        ffn_kernel,
        name="ffn",
        grid=(groups,),
        out_shape=jax.ShapeDtypeStruct(rows.shape, BF16),
        in_specs=[
            pl.BlockSpec(rows.shape, lambda g: (0, 0)),
            pl.BlockSpec((1, width, quarter), lambda g: (g, 0, 0)),
            pl.BlockSpec((1, width, quarter), lambda g: (g, 0, 0)),
            pl.BlockSpec((1, quarter, width), lambda g: (g, 0, 0)),
        ],
        out_specs=pl.BlockSpec(rows.shape, lambda g: (0, 0)),
        scratch_shapes=[pltpu.VMEM(rows.shape, F32)],
        cost_estimate=pl.CostEstimate(
            flops=8_000_000_000, bytes_accessed=17_000_000, transcendentals=0
        ),
        compiler_params=pltpu.CompilerParams(
            dimension_semantics=("arbitrary",), vmem_limit_bytes=56 * 2**20
        ),
    )(rows, w_gate, w_up, w_down)


def head_pairs(recur_w, inject_w):
    heads, dim, _ = recur_w.shape

    def paired(w):
        zero = jnp.zeros((heads // 2, dim, dim), w.dtype)
        top = jnp.concatenate([w[0::2], zero], axis=2)
        bottom = jnp.concatenate([zero, w[1::2]], axis=2)
        return jnp.concatenate([top, bottom], axis=1)

    return jnp.concatenate([paired(recur_w), paired(inject_w)], axis=2)


def body(
    mix_tokens,
    mix_gain,
    w_branch,
    w_gate_branch,
    conv_taps,
    recur_gate_w,
    inject_gate_w,
    decay_logit,
    decay_kick,
    w_mix_out,
    moe_tokens,
    moe_gain,
    expert_ids,
    route_weight,
    expert_gate_w,
    expert_up_w,
    expert_down_w,
):
    full_gate = lax.all_gather(expert_gate_w[0], "tp")
    full_up = lax.all_gather(expert_up_w[0], "tp")
    full_down = lax.all_gather(expert_down_w[0], "tp")
    rows, outgoing, table = pre(
        mix_tokens, mix_gain[None, :], moe_tokens, moe_gain[None, :], expert_ids, route_weight
    )
    width = outgoing.shape[1]
    arrived = lax.all_to_all(
        outgoing.reshape(64, 8, width), EP, split_axis=0, concat_axis=0, tiled=True
    ).reshape(-1, width)
    blocks, rim = gather_rows(rows)
    cols = w_branch.shape[1]
    widen = (
        jnp.arange(cols, dtype=jnp.int32)[None, :] // 64 == jnp.arange(8, dtype=jnp.int32)[:, None]
    ).astype(BF16)
    gate, state, decay, last = mid(
        blocks,
        rim,
        w_branch,
        w_gate_branch,
        conv_taps.astype(F32),
        head_pairs(recur_gate_w, inject_gate_w),
        jax.nn.softplus(-decay_logit)[None, :],
        decay_kick,
        widen,
    )
    carry = carried_state(last).reshape(1, cols)
    partial = out_partial(state, decay, gate, carry, w_mix_out)
    done = ffn(arrived, full_gate, full_up, full_down)
    returned = lax.all_to_all(
        done.reshape(64, 8, width), EP, split_axis=0, concat_axis=0, tiled=True
    ).reshape(-1, width)
    partial, done = lax.optimization_barrier((partial, done))
    mixer_out = sum_over_tp(partial)
    expert_out = dot(table, returned).astype(BF16)
    return (mixer_out, expert_out)


def solution(mesh):
    torus = Mesh(mesh.devices.reshape(8, 4, 2, mesh.shape["tp"]), EP_TP)
    placed = (
        P(EP_TP, None),
        P(),
        P(None, "tp"),
        P(None, "tp"),
        P(None, "tp"),
        P("tp", None, None),
        P("tp", None, None),
        P("tp"),
        P(EP, "tp"),
        P("tp", None),
        P(EP_TP, None),
        P(),
        P(EP_TP, None),
        P(EP_TP, None),
        P(EP, None, "tp"),
        P(EP, None, "tp"),
        P(EP, "tp", None),
    )
    return jax.shard_map(
        body,
        mesh=torus,
        in_specs=placed,
        out_specs=(P(EP_TP, None), P(EP_TP, None)),
        check_vma=False,
    )
```
